32 devices in a mesh: rep: 2 (over x), fs: 4 (over z), tp: 4 (over y, core).
Axes of the slice: x: 2, y: 2, z: 4, core: 2. Of those that a mesh axis runs over, the one named last changes fastest.
Arguments:
- tokens: bfloat16 [8, 1024, 2048], P(('rep', 'fs')), may hold values from -6 to 6
- mix_gain: bfloat16 [2048], replicated, may hold values from 0.099609375 to 1.8984375
- value_weight: bfloat16 [2048, 1024], P('fs', 'tp'), may hold values from -0.125 to 0.125
- gate_weight: bfloat16 [2048, 1024], P('fs', 'tp'), may hold values from -0.125 to 0.125
- mix_taps: bfloat16 [31, 1024], P(None, 'tp'), may hold values from -1 to 1
- head_gain: bfloat16 [1024], P('tp'), may hold values from 0.099609375 to 1.8984375
- out_weight: bfloat16 [1024, 2048], P('fs', 'tp'), may hold values from -0.1875 to 0.1875
- ffn_gain: bfloat16 [2048], replicated, may hold values from 0.099609375 to 1.8984375
- ffgate_weight: bfloat16 [2048, 6144], P('fs', 'tp'), may hold values from -0.125 to 0.125
- up_weight: bfloat16 [2048, 6144], P('fs', 'tp'), may hold values from -0.125 to 0.125
- ff_taps: bfloat16 [3, 6144], P(None, 'tp'), may hold values from -3.5 to 3.5
- down_weight: bfloat16 [2048, 6144], P('fs', 'tp'), may hold values from -0.078125 to 0.078125
Outputs:
- layer_out: bfloat16 [8, 1024, 2048], P(('rep', 'fs'), 'tp')
The draws below stay inside these ranges and needn't reach their ends.
All inputs are finite; a program needn't handle non-finite values.
Results may differ from the reference program's by a relative error of at most 0.01.
Values may be sent and summed in bfloat16 or wider, within the bound.
No kernel may reach another device: no remote copies, remote signals or barrier semaphores. Data moves between devices by JAX's collectives and lax.ppermute only.
A program may use at most 128 MiB of HBM per device.

```python
import jax
import jax.numpy as jnp
from jax import lax

D = 2048
CW = 1024
FF = 6144
HEAD = 128
KW = 31
KF = 3
LEN = 1024
BATCH = 8


def steps_of(stream_key, shape, cuts, smallest, largest):
    level = 1.0
    for dim, parts in cuts:
        draws = jax.random.uniform(jax.random.fold_in(jax.random.fold_in(stream_key, 6), dim), (parts,), jnp.float32, smallest / len(cuts), largest / len(cuts))
        level = level * jnp.repeat(jnp.exp(draws), shape[dim] // parts).reshape((-1,) + (1,) * (len(shape) - 1 - dim))
    return level


def normal_values(stream_key, shape, scale, bound, pieces=(), kind=jnp.bfloat16):
    level = steps_of(stream_key, shape, pieces, -0.22, 0.18) if pieces else 1.0
    array = jax.random.normal(stream_key, shape, jnp.float32) * scale * level
    return jnp.minimum(jnp.maximum(array, -bound), bound).astype(kind)


def setup_inputs(seed: int = 0) -> dict:
    key_of = jax.random.split(jax.random.key(seed), 13)
    tokens = normal_values(key_of[0], (BATCH, LEN, D), 1.0, 6.0, ((0, 8),))
    mix_gain = jnp.clip(1.0 + 0.18 * jax.random.normal(key_of[1], (D,), jnp.float32), 0.099609375, 1.8984375).astype(jnp.bfloat16)
    value_weight = normal_values(key_of[2], (D, CW), D ** -0.5, 0.125, ((0, 4), (1, 4)))
    gate_weight = normal_values(key_of[3], (D, CW), D ** -0.5, 0.125, ((0, 4), (1, 4)))
    mix_taps = normal_values(key_of[4], (KW, CW), KW ** -0.5, 1.0, ((1, 4),))
    head_gain = jnp.clip(1.0 + 0.18 * jax.random.normal(key_of[5], (CW,), jnp.float32), 0.099609375, 1.8984375).astype(jnp.bfloat16)
    out_weight = normal_values(key_of[6], (CW, D), CW ** -0.5, 0.1875, ((0, 4), (1, 4)))
    ffn_gain = jnp.clip(1.0 + 0.18 * jax.random.normal(key_of[7], (D,), jnp.float32), 0.099609375, 1.8984375).astype(jnp.bfloat16)
    ffgate_weight = normal_values(key_of[8], (D, FF), D ** -0.5, 0.125, ((0, 4), (1, 4)))
    up_weight = normal_values(key_of[9], (D, FF), D ** -0.5, 0.125, ((0, 4), (1, 4)))
    ff_taps = normal_values(key_of[10], (KF, FF), KF ** -0.5, 3.5, ((1, 4),))
    down_weight = normal_values(key_of[11], (D, FF), FF ** -0.5, 0.078125, ((0, 4), (1, 4)))
    return {"tokens": tokens, "mix_gain": mix_gain, "value_weight": value_weight, "gate_weight": gate_weight, "mix_taps": mix_taps, "head_gain": head_gain, "out_weight": out_weight, "ffn_gain": ffn_gain, "ffgate_weight": ffgate_weight, "up_weight": up_weight, "ff_taps": ff_taps, "down_weight": down_weight}


norm_floor = 0.01

def row_norm(floats_in, scales):
    floats = floats_in.astype(jnp.float32)
    scaled = floats * lax.rsqrt(lax.optimization_barrier(jnp.mean(floats * floats, axis=-1, keepdims=True)) + norm_floor)
    return (scaled * scales.astype(jnp.float32)).astype(jnp.bfloat16)

def causal_conv(signal, kernel_taps):
    reach = kernel_taps.shape[0]
    length = signal.shape[0]
    padded = jnp.pad(signal, ((reach - 1, 0), (0, 0)))
    summed = padded[0:length] * kernel_taps[0]
    for offset in range(1, reach):
        summed = summed + padded[offset:offset + length] * kernel_taps[offset]
    return summed

def head_norm(signal, scales):
    length = signal.shape[0]
    grouped = signal.reshape(length, signal.shape[1] // HEAD, HEAD)
    centre = grouped - lax.optimization_barrier(jnp.mean(grouped, axis=-1, keepdims=True))
    spread = lax.optimization_barrier(jnp.mean(centre * centre, axis=-1, keepdims=True))
    normal = (centre * lax.rsqrt(spread + norm_floor)).reshape(signal.shape)
    return normal * scales.astype(jnp.float32)

def reference(tokens, mix_gain, value_weight, gate_weight, mix_taps, head_gain, out_weight, ffn_gain, ffgate_weight, up_weight, ff_taps, down_weight):

    def sublayers(sequence):
        normed = row_norm(sequence, mix_gain)
        values = jnp.dot(normed, value_weight, preferred_element_type=jnp.float32)
        gating = jnp.dot(normed, gate_weight, preferred_element_type=jnp.float32)
        glu_out = values * jax.nn.sigmoid(gating)
        mixed_pos = causal_conv(glu_out, mix_taps.astype(jnp.float32))
        head_out = jax.nn.silu(head_norm(mixed_pos, head_gain)).astype(jnp.bfloat16)
        hidden = (sequence.astype(jnp.float32) + jnp.dot(head_out, out_weight, preferred_element_type=jnp.float32)).astype(jnp.bfloat16)
        normed_ffn = row_norm(hidden, ffn_gain)
        ffgate = jnp.dot(normed_ffn, ffgate_weight, preferred_element_type=jnp.float32)
        ff_up = jnp.dot(normed_ffn, up_weight, preferred_element_type=jnp.float32)
        product = (jax.nn.silu(causal_conv(ffgate, ff_taps.astype(jnp.float32))) * ff_up).astype(jnp.bfloat16)
        down_sum = lax.dot_general(product, down_weight, (((1,), (1,)), ((), ())), preferred_element_type=jnp.float32)
        return (hidden.astype(jnp.float32) + down_sum).astype(jnp.bfloat16)
    return lax.map(sublayers, tokens)
```

```python
import jax
import jax.numpy as jnp
from jax import lax
from jax.sharding import PartitionSpec as P


HEAD = 128


norm_floor = 0.01


def row_norm(floats_in, scales):
    floats = floats_in.astype(jnp.float32)
    scaled = floats * lax.rsqrt(jnp.mean(floats * floats, axis=-1, keepdims=True) + norm_floor)
    return (scaled * scales.astype(jnp.float32)).astype(jnp.bfloat16)


def causal_conv(signal, kernel_taps):
    reach = kernel_taps.shape[0]
    length = signal.shape[0]
    padded = jnp.pad(signal, ((reach - 1, 0), (0, 0)))
    summed = padded[0:length] * kernel_taps[0]
    for offset in range(1, reach):
        summed = summed + padded[offset : offset + length] * kernel_taps[offset]
    return summed


def head_norm(signal, scales):
    length = signal.shape[0]
    grouped = signal.reshape(length, signal.shape[1] // HEAD, HEAD)
    centre = grouped - jnp.mean(grouped, axis=-1, keepdims=True)
    spread = jnp.mean(centre * centre, axis=-1, keepdims=True)
    normal = (centre * lax.rsqrt(spread + norm_floor)).reshape(signal.shape)
    return normal * scales.astype(jnp.float32)


def ring_send(piece, steps, axis):
    size = lax.axis_size(axis)
    return lax.ppermute(piece, axis, [(i, (i + steps) % size) for i in range(size)])


def swap(piece, axis, bit):
    return lax.ppermute(piece, axis, [(i, i ^ bit) for i in range(lax.axis_size(axis))])


def bits_of(axis):
    size = lax.axis_size(axis)
    assert size & (size - 1) == 0
    return [1 << i for i in range(size.bit_length() - 1)]


def columns_gather(block, axis):
    place = lax.axis_index(axis)
    held = [(0, block)]
    for bit in reversed(bits_of(axis)):
        held = held + [(far ^ bit, swap(piece, axis, bit)) for far, piece in held]
    width = block.shape[1]
    whole = jnp.zeros((block.shape[0], width * len(held)), block.dtype)
    for far, piece in held:
        whole = lax.dynamic_update_slice_in_dim(whole, piece, (place ^ far) * width, 1)
    return whole


def rows_scatter(block, axis):
    place = lax.axis_index(axis)
    size = lax.axis_size(axis)
    count = block.shape[0] // size
    rows = block.reshape(size, count, block.shape[1])
    for bit in bits_of(axis):
        pairs = rows.reshape(rows.shape[0] // 2, 2, count, rows.shape[2])
        mine = (place // bit) % 2
        kept = lax.dynamic_index_in_dim(pairs, mine, 1, keepdims=False)
        sent = lax.dynamic_index_in_dim(pairs, 1 - mine, 1, keepdims=False)
        rows = kept.astype(jnp.float32) + swap(sent.astype(jnp.bfloat16), axis, bit).astype(
            jnp.float32
        )
    return rows[0]


def gather_rows(group, arrived, depth, gates=()):
    ring, copies = lax.axis_size("fs"), lax.axis_size("rep")
    copy = lax.axis_index("rep")
    moving, found = [], [[[(0, shard)]] for shard, _ in group]
    for i, (shard, parts) in enumerate(group):
        share = shard.shape[0] // copies
        count = share // parts
        for part in range(parts):
            piece = lax.dynamic_slice_in_dim(shard, copy * share + part * count, count, 0)
            moving.append([i, share, part * count, piece])
    for step in range(1, ring):
        for pieces in found:
            pieces.append([])
        for item in moving:
            i, share, offset, piece = item
            if len(arrived) >= depth:
                piece, _ = lax.optimization_barrier((piece, arrived[-depth]))
            if step <= len(gates):
                piece, _ = lax.optimization_barrier((piece, gates[step - 1]))
            piece = ring_send(piece, 1, "fs")
            item[3] = piece
            arrived.append(piece)
            found[i][step].append((copy * share + offset, piece))
            for other in range(1, copies):
                start = (copy - other) % copies * share + offset
                found[i][step].append((start, ring_send(piece, other, "rep")))
    return found


def put_rows(steps, shard_rows, first=0, last=None):
    ring, here = lax.axis_size("fs"), lax.axis_index("fs")
    steps = list(enumerate(steps))[first:last]
    whole = jnp.zeros((shard_rows * len(steps), steps[0][1][0][1].shape[1]), jnp.bfloat16)
    for step, pieces in steps:
        if len(steps) == ring:
            base = (here - step) % ring * shard_rows
        else:
            base = (step - first) * shard_rows
        for start, piece in pieces:
            whole = lax.dynamic_update_slice_in_dim(whole, piece, base + start, 0)
    return whole


def on_device(
    tokens,
    mix_gain,
    value_weight,
    gate_weight,
    mix_taps,
    head_gain,
    out_weight,
    ffn_gain,
    ffgate_weight,
    up_weight,
    ff_taps,
    down_weight,
):
    sequence = tokens[0]
    width = sequence.shape[1]
    arrived = []
    value_rows, gate_rows = gather_rows(((value_weight, 1), (gate_weight, 1)), arrived, DEPTH)
    (out_rows,) = gather_rows(((out_weight, 1),), [], DEPTH)
    ffgate_rows, up_rows = gather_rows(((ffgate_weight, 1), (up_weight, 1)), arrived, DEPTH)
    shard_rows = ffgate_weight.shape[0]
    normed = row_norm(sequence, mix_gain)
    values = jnp.dot(normed, put_rows(value_rows, shard_rows), preferred_element_type=jnp.float32)
    gating = jnp.dot(normed, put_rows(gate_rows, shard_rows), preferred_element_type=jnp.float32)
    glu_out = values * jax.nn.sigmoid(gating)
    mixed_pos = causal_conv(glu_out, mix_taps.astype(jnp.float32))
    head_out = jax.nn.silu(head_norm(mixed_pos, head_gain)).astype(jnp.bfloat16)
    out_full = put_rows(out_rows, out_weight.shape[0])
    out_cols = out_full.shape[1]
    heads = columns_gather(head_out, "tp")
    mixer_sum = jnp.dot(heads, out_full, preferred_element_type=jnp.float32)
    own_cols = lax.dynamic_slice_in_dim(sequence, lax.axis_index("tp") * out_cols, out_cols, 1)
    hidden_cols = (own_cols.astype(jnp.float32) + mixer_sum).astype(jnp.bfloat16)
    full_rows = columns_gather(hidden_cols, "tp")
    normed_ffn = lax.optimization_barrier(row_norm(full_rows, ffn_gain))
    ffgate = jnp.dot(normed_ffn, put_rows(ffgate_rows, shard_rows), preferred_element_type=jnp.float32)
    gate_part = lax.optimization_barrier(
        jax.nn.silu(causal_conv(ffgate, ff_taps.astype(jnp.float32)))
    )
    up_rows[-1] = [
        (start, lax.optimization_barrier((piece, gate_part[:8, :128]))[0])
        for start, piece in up_rows[-1]
    ]
    ff_up = jnp.dot(normed_ffn, put_rows(up_rows, shard_rows), preferred_element_type=jnp.float32)
    product = lax.optimization_barrier((gate_part * ff_up).astype(jnp.bfloat16))
    own_count = sequence.shape[0] // lax.axis_size("tp")
    own_rows = lax.dynamic_slice_in_dim(full_rows, lax.axis_index("tp") * own_count, own_count, 0)
    summed_rows = jnp.zeros((own_count, width), jnp.float32)
    (down_steps,) = gather_rows(((down_weight, 2),), arrived, DEPTH, (normed_ffn[:8, :128],))
    ring, here = lax.axis_size("fs"), lax.axis_index("fs")
    down_rows = down_weight.shape[0]
    for first, last in [(0, 2)] + [(step, step + 1) for step in range(2, ring)]:
        partial = lax.dot_general(
            product,
            put_rows(down_steps, down_rows, first, last),
            (((1,), (1,)), ((), ())),
            preferred_element_type=jnp.float32,
        )
        sums = rows_scatter(partial, "tp")
        for step in range(first, last):
            summed_rows = lax.dynamic_update_slice_in_dim(
                summed_rows,
                sums[:, (step - first) * down_rows : (step - first + 1) * down_rows],
                (here - step) % ring * down_rows,
                1,
            )
    return (own_rows.astype(jnp.float32) + summed_rows).astype(jnp.bfloat16)[None]


DEPTH = 3


def solution(mesh):
    placed = (
        P(("rep", "fs"), None, None),
        P(),
        P("fs", "tp"),
        P("fs", "tp"),
        P(None, "tp"),
        P("tp"),
        P("fs", "tp"),
        P(),
        P("fs", "tp"),
        P("fs", "tp"),
        P(None, "tp"),
        P("fs", "tp"),
    )
    return jax.shard_map(
        on_device,
        mesh=mesh,
        in_specs=placed,
        out_specs=P(("rep", "fs"), "tp", None),
        check_vma=False,
    )
```
